256 devices in a mesh: ep: 16 (over y, x), tp: 16 (over z, core).
Axes of the slice: x: 4, y: 4, z: 8, core: 2. Of those that a mesh axis runs over, the one named last changes fastest.
Arguments:
- tokens: bfloat16 [65536, 2048], P(('ep', 'tp')), may hold values from -6 to 6
- norm_gain: float32 [2048], replicated, may hold values from 0.1 to 1.9
- expert_ids: int32 [65536, 2], P(('ep', 'tp')), may hold values from 0 to 15, all different within a row; in each aligned block of 256 rows (0 to 255, 256 to 511, ...) at most 64 rows name the same one
- gate_weights: float32 [65536, 2], P(('ep', 'tp')), may hold values from 0.2 to 1
- w_gate: bfloat16 [16, 2048, 1024], P('ep', None, 'tp'), may hold values from -0.125 to 0.125
- w_up: bfloat16 [16, 2048, 1024], P('ep', None, 'tp'), may hold values from -0.125 to 0.125
- w_down: bfloat16 [16, 2048, 1024], P('ep', None, 'tp'), may hold values from -0.1875 to 0.1875
- dense_gate: bfloat16 [2048, 256], P('ep'), may hold values from -0.125 to 0.125
- dense_up: bfloat16 [2048, 256], P('ep'), may hold values from -0.125 to 0.125
- dense_down: bfloat16 [256, 2048], P(None, 'ep'), may hold values from -0.375 to 0.375
- mix_vector: float32 [2048], replicated, may hold values from -0.125 to 0.125
Outputs:
- mixed: bfloat16 [65536, 2048], P(('ep', 'tp'))
The draws below stay inside these ranges and needn't reach their ends.
Inputs may be any that keep to these rules, and one draw needn't show every extreme that they name: `expert_ids`: A row names 2 different experts. In the rows of one device (aligned blocks of 256 rows) each expert is named by at most 64 rows, a bound that some block reaches.
All inputs are finite; a program needn't handle non-finite values.
Results may differ from the reference program's by a relative error of at most 0.0075.
Values may be sent and summed in bfloat16 or wider, within the bound.
No kernel may reach another device: no remote copies, remote signals or barrier semaphores. Data moves between devices by JAX's collectives and lax.ppermute only.
A program may use at most 320 MiB of HBM per device.

```python
import math
import jax
import jax.numpy as jnp
import numpy as np
from jax import lax

D = 2048
FF = 1024
FS = 256
TOPK = 2
TOK_DEV = 256
EXPERTS = 16
CAP = 64
TOKENS = 65536


def steps_of(own_key, shape, pieces, low, largest):
    def one(axis_at, parts):
        heights = jax.random.uniform(jax.random.fold_in(jax.random.fold_in(own_key, 6), axis_at), (parts,), jnp.float32, low / len(pieces), largest / len(pieces))
        return jnp.repeat(jnp.exp(heights), shape[axis_at] // parts).reshape((-1,) + (1,) * (len(shape) - axis_at - 1))

    level = one(*pieces[0])
    for cut in pieces[1:]:
        level = level * one(*cut)
    return level


def shared_out(stream_key, own, number, rows, amount, top, limit, slope):
    order = jax.random.permutation(stream_key, amount)
    crowded, ordinary = load_shares(amount, rows * top, limit, slope, True), load_shares(amount, rows * top, limit, slope, False)
    places = jnp.arange(amount)

    def named(tallies, turn):
        used = int((tallies > 0).sum())
        fixed = max(1, used // 4)
        passed = fixed + (places - fixed + turn * (used - fixed)) % max(1, amount - fixed)
        return jnp.zeros((amount,), jnp.int32).at[order[jnp.where(places < fixed, places, passed)]].set(jnp.asarray(tallies, jnp.int32))

    tallies = jnp.where(number % 4 == 0, named(crowded, number // 4), named(ordinary, number - number // 4 - 1))
    mixed = jax.random.permutation(jax.random.fold_in(own, 3), amount)
    source_of, sink = mixed[0:amount // 2 * 2:2], mixed[1:amount // 2 * 2:2]
    margin = jnp.minimum(tallies[source_of] - 1, limit - tallies[sink]) // 2
    margin = jnp.where((source_of == order[0]) | (sink == order[0]) | (tallies[sink] == 0), 0, jnp.maximum(margin, 0))
    passed = jax.random.randint(jax.random.fold_in(own, 4), (amount // 2,), 0, 1 << 20) % (margin + 1)
    tallies = tallies.at[source_of].add(-passed).at[sink].add(passed)
    labels = jnp.searchsorted(jnp.cumsum(tallies), jnp.arange(rows * top), side="right").astype(jnp.int32)
    table = labels.reshape(top, rows).T
    table = table[jax.random.permutation(jax.random.fold_in(own, 1), rows)]
    turn = jax.random.randint(jax.random.fold_in(own, 2), (rows, 1), 0, top)
    return jnp.take_along_axis(table, (jnp.arange(top)[None, :] + turn) % top, axis=1)


def load_shares(amount, total, bound, slope, full):
    portions = [(1 << 20) // math.isqrt(standing ** slope) + 1 for standing in range(1, amount + 1)]
    largest = bound if full else min(bound, max(-(-total // amount), total * portions[0] // sum(portions)))
    least = 1 if total - largest >= amount - 1 else 0
    counts, surplus = [largest] + [least] * (amount - 1), total - largest - least * (amount - 1)
    while surplus > 0:
        free = [i for i in range(1, amount) if counts[i] < largest] or [i for i in range(1, amount) if counts[i] < bound]
        pool, left = sum([portions[i] for i in free]), surplus
        for i in free:
            addition = min(bound - counts[i], max(1, left * portions[i] // pool), surplus)
            counts[i] = counts[i] + addition
            surplus = surplus - addition
    return np.array(counts)


def normal_values(rng, extent, spread, limit, pieces=(), held_as=jnp.bfloat16):
    values = spread * jax.random.normal(rng, extent, jnp.float32)
    if pieces:
        values = values * steps_of(rng, extent, pieces, -0.22, 0.18)
    return jnp.clip(values, -limit, limit).astype(held_as)


def setup_inputs(seed: int = 0) -> dict:
    keys = jax.random.split(jax.random.key(seed), 12)
    tokens = normal_values(keys[0], (TOKENS, D), 1.0, 6.0, ((0, 256),))
    norm_gain = jnp.clip(1.0 + 0.18 * jax.random.normal(keys[1], (D,), jnp.float32), 0.1, 1.9)
    expert_ids_keys = jax.random.split(jax.random.fold_in(keys[2], 1), TOKENS // TOK_DEV)
    expert_ids_turns = jax.random.permutation(jax.random.fold_in(keys[2], 3), TOKENS // TOK_DEV)
    expert_ids = jax.vmap(lambda own, number: shared_out(jax.random.fold_in(keys[2], 2), own, number, TOK_DEV, EXPERTS, TOPK, CAP, 2))(expert_ids_keys, expert_ids_turns).reshape((TOKENS, TOPK))
    gate_weights = jnp.clip(0.2 + 0.8 * jax.random.uniform(keys[3], (TOKENS, TOPK), jnp.float32) ** steps_of(keys[3], (TOKENS, TOPK), ((0, 256),), -0.2, 0.2), 0.2, 1.0)
    w_gate = normal_values(keys[4], (EXPERTS, D, FF), D ** -0.5, 0.125, ((0, 16), (2, 16)))
    w_up = normal_values(keys[5], (EXPERTS, D, FF), D ** -0.5, 0.125, ((0, 16), (2, 16)))
    w_down = normal_values(keys[6], (EXPERTS, D, FF), FF ** -0.5, 0.1875, ((0, 16), (2, 16)))
    dense_gate = normal_values(keys[7], (D, FS), D ** -0.5, 0.125, ((0, 16),))
    dense_up = normal_values(keys[8], (D, FS), D ** -0.5, 0.125, ((0, 16),))
    dense_down = normal_values(keys[9], (FS, D), FS ** -0.5, 0.375, ((1, 16),))
    mix_vector = normal_values(keys[10], (D,), D ** -0.5, 0.125, (), jnp.float32)
    return dict(tokens=tokens, norm_gain=norm_gain, expert_ids=expert_ids, gate_weights=gate_weights, w_gate=w_gate, w_up=w_up, w_down=w_down, dense_gate=dense_gate, dense_up=dense_up, dense_down=dense_down, mix_vector=mix_vector)


eps = 1e-06

def reference(tokens, norm_gain, expert_ids, gate_weights, w_gate, w_up, w_down, dense_gate, dense_up, dense_down, mix_vector):
    values = tokens.astype(jnp.float32)
    scale = lax.rsqrt(lax.optimization_barrier(jnp.mean(values * values, axis=1, keepdims=True)) + eps)
    normed = (values * scale * norm_gain).astype(jnp.bfloat16)
    blocks = TOKENS // TOK_DEV
    pairs = TOK_DEV * TOPK
    ids = expert_ids.reshape(blocks, pairs)
    onehot = (ids[:, :, None] == jnp.arange(EXPERTS, dtype=jnp.int32)[None, None, :]).astype(jnp.int32)
    before = jnp.cumsum(onehot, axis=1) - onehot
    slot = lax.optimization_barrier(jnp.sum(before * onehot, axis=2)).astype(jnp.int32)
    dest = (ids * CAP + slot).astype(jnp.int32)
    block_rows = jnp.arange(blocks, dtype=jnp.int32)[:, None]
    token_index = block_rows * TOK_DEV + (jnp.arange(pairs, dtype=jnp.int32) // TOPK)[None, :]
    table = jnp.full((blocks, EXPERTS * CAP), TOKENS, jnp.int32)
    table = table.at[block_rows, dest].set(token_index.astype(jnp.int32))
    weight_table = jnp.zeros((blocks, EXPERTS * CAP), jnp.float32)
    weight_table = weight_table.at[block_rows, dest].set(gate_weights.reshape(blocks, pairs))
    padded = jnp.concatenate([normed, jnp.zeros((1, D), jnp.bfloat16)], axis=0)

    def one_expert(total, expert):
        index = lax.dynamic_slice_in_dim(table, (expert * CAP).astype(jnp.int32), CAP, 1).reshape(-1)
        weight = lax.dynamic_slice_in_dim(weight_table, (expert * CAP).astype(jnp.int32), CAP, 1).reshape(-1)
        rows = padded[index]
        gate = jnp.dot(rows, w_gate[expert], preferred_element_type=jnp.float32)
        upper = jnp.dot(rows, w_up[expert], preferred_element_type=jnp.float32)
        hidden = (jax.nn.silu(gate) * upper).astype(jnp.bfloat16)
        result = jnp.dot(hidden, w_down[expert].T, preferred_element_type=jnp.float32).astype(jnp.bfloat16)
        return (total.at[index].add(weight[:, None] * result.astype(jnp.float32)), None)
    start = jnp.zeros((TOKENS + 1, D), jnp.float32)
    routed, unused = lax.scan(one_expert, start, jnp.arange(EXPERTS, dtype=jnp.int32))
    routed = routed[:TOKENS]
    dense_g = jnp.dot(normed, dense_gate, preferred_element_type=jnp.float32)
    dense_u = jnp.dot(normed, dense_up, preferred_element_type=jnp.float32)
    dense_hidden = (jax.nn.silu(dense_g) * dense_u).astype(jnp.bfloat16)
    dense_out = jnp.dot(dense_hidden, dense_down, preferred_element_type=jnp.float32)
    mix = jax.nn.sigmoid(lax.optimization_barrier(jnp.sum(normed.astype(jnp.float32) * mix_vector, axis=1)))
    return (routed + mix[:, None] * dense_out).astype(jnp.bfloat16)
```

```python
import functools

import jax
import jax.numpy as jnp
from jax import lax
from jax.experimental import pallas as pl
from jax.experimental.pallas import tpu as pltpu
from jax.sharding import Mesh
from jax.sharding import PartitionSpec as P

EP = ("ep_0", "ep_1")
EP_TP = ("ep_0", "ep_1", "tp")
EPS = 1e-06
PIECES = 4
NT = (((1,), (1,)), ((), ()))


def cost(flops, moved):
    return pl.CostEstimate(flops=int(flops), bytes_accessed=int(moved), transcendentals=0)


def dispatch_kernel(groups, cap, tok_ref, gain_ref, ids_ref, buf_ref, normed_ref, dest_ref):
    step = pl.program_id(0)
    count = tok_ref.shape[0]

    @pl.when(step == 0)
    def _():
        values = tok_ref[...].astype(jnp.float32)
        scale = lax.rsqrt(jnp.mean(values * values, axis=1, keepdims=True) + EPS)
        normed_ref[...] = (values * scale * gain_ref[...]).astype(jnp.bfloat16)
        ids = ids_ref[...]
        expert = lax.broadcasted_iota(jnp.int32, (groups, count), 0)
        hot = [jnp.where(ids[k : k + 1, :] == expert, 1.0, 0.0) for k in range(2)]
        row = lax.broadcasted_iota(jnp.int32, (count, count), 0)
        col = lax.broadcasted_iota(jnp.int32, (count, count), 1)
        earlier = jnp.where(row < col, 1.0, 0.0).astype(jnp.bfloat16)
        before = jnp.dot((hot[0] + hot[1]).astype(jnp.bfloat16), earlier, preferred_element_type=jnp.float32)
        slots = [jnp.sum(before * h, axis=0, keepdims=True).astype(jnp.int32) for h in hot]
        dest_ref[...] = jnp.concatenate(
            [ids[k : k + 1, :] * cap + slots[k] for k in range(2)] + [jnp.zeros((6, count), jnp.int32)], axis=0
        )

    rows = buf_ref.shape[0]
    place = step * rows + lax.broadcasted_iota(jnp.int32, (rows, count), 0)
    chosen = (place == dest_ref[0:1, :]) | (place == dest_ref[1:2, :])
    pick = jnp.where(chosen, 1.0, 0.0).astype(jnp.bfloat16)
    buf_ref[...] = jnp.dot(pick, normed_ref[...], preferred_element_type=jnp.float32).astype(jnp.bfloat16)


def dispatch(tokens, gain, ids_t, groups, cap):
    count, width = tokens.shape
    total, steps = groups * cap, 4
    return pl.pallas_call(
        functools.partial(dispatch_kernel, groups, cap),
        grid=(steps,),
        in_specs=[
            pl.BlockSpec((count, width), lambda i: (0, 0)),
            pl.BlockSpec((1, width), lambda i: (0, 0)),
            pl.BlockSpec((2, count), lambda i: (0, 0)),
        ],
        out_specs=[
            pl.BlockSpec((total // steps, width), lambda i: (i, 0)),
            pl.BlockSpec((count, width), lambda i: (0, 0)),
            pl.BlockSpec((8, count), lambda i: (0, 0)),
        ],
        out_shape=[
            jax.ShapeDtypeStruct((total, width), jnp.bfloat16),
            jax.ShapeDtypeStruct((count, width), jnp.bfloat16),
            jax.ShapeDtypeStruct((8, count), jnp.int32),
        ],
        cost_estimate=cost(2 * total * count * width, 8 * total * width),
        name="dispatch",
    )(tokens, gain.reshape(1, width), ids_t)


def weigh_kernel(dest_ref, gates_ref, hi_ref, lo_ref):
    count, total = hi_ref.shape
    dest = dest_ref[...].astype(jnp.float32).T
    gates = jnp.concatenate([gates_ref[...], jnp.zeros((6, count), jnp.float32)], axis=0).T
    place = lax.broadcasted_iota(jnp.int32, (count, total), 1).astype(jnp.float32)
    weight = sum(jnp.where(place == dest[:, k : k + 1], gates[:, k : k + 1], 0.0) for k in range(2))
    hi = weight.astype(jnp.bfloat16)
    hi_ref[...] = hi
    lo_ref[...] = (weight - hi.astype(jnp.float32)).astype(jnp.bfloat16)


def weigh(dest, gates_t, total):
    count = gates_t.shape[1]
    shape = jax.ShapeDtypeStruct((count, total), jnp.bfloat16)
    return pl.pallas_call(
        weigh_kernel,
        out_shape=[shape, shape],
        cost_estimate=cost(1e9, 4 * count * total),
        name="weigh",
    )(dest, gates_t)


def hidden_kernel(rows_ref, gate_ref, up_ref, out_ref):
    rows = rows_ref[...]
    gate = lax.dot_general(rows, gate_ref[...], NT, preferred_element_type=jnp.float32)
    upper = lax.dot_general(rows, up_ref[...], NT, preferred_element_type=jnp.float32)
    out_ref[...] = (jax.nn.silu(gate) * upper).astype(jnp.bfloat16)


def hidden_units(rows, both):
    total, width = rows.shape
    units = both.shape[0]
    block = 256
    return pl.pallas_call(
        hidden_kernel,
        grid=(units // block,),
        in_specs=[
            pl.BlockSpec((total, width), lambda i: (0, 0)),
            pl.BlockSpec((block, width), lambda i: (i, 0)),
            pl.BlockSpec((block, width), lambda i: (i, 1)),
        ],
        out_specs=pl.BlockSpec((total, block), lambda i: (0, i)),
        out_shape=jax.ShapeDtypeStruct((total, units), jnp.bfloat16),
        cost_estimate=cost(4 * total * width * units, 2 * total * width + 4 * units * width + 2 * total * units),
        name="hidden_units",
    )(rows, both, both)


def down_kernel(hidden_ref, down_ref, out_ref):
    out_ref[...] = jnp.dot(hidden_ref[...], down_ref[...], preferred_element_type=jnp.float32).astype(jnp.bfloat16)


def down_piece(hidden, down, at, pieces):
    total, units = hidden.shape
    wide = down.shape[1] // pieces
    return pl.pallas_call(
        down_kernel,
        grid=(2,),
        in_specs=[
            pl.BlockSpec((total // 2, units), lambda i: (i, 0)),
            pl.BlockSpec((units, wide), lambda i: (0, at)),
        ],
        out_specs=pl.BlockSpec((total // 2, wide), lambda i: (i, 0)),
        out_shape=jax.ShapeDtypeStruct((total, wide), jnp.bfloat16),
        cost_estimate=cost(2 * total * wide * units, 2 * total * units + 2 * units * wide + 2 * total * wide),
        name=f"down_{at}",
    )(hidden, down)


def side_kernel(normed_ref, vector_ref, both_ref, down_ref, out_ref):
    normed = normed_ref[...]
    half = both_ref.shape[1] // 2
    both = jnp.dot(normed, both_ref[...], preferred_element_type=jnp.float32)
    hidden = (jax.nn.silu(both[:, :half]) * both[:, half:]).astype(jnp.bfloat16)
    mix = jax.nn.sigmoid(jnp.sum(normed.astype(jnp.float32) * vector_ref[...], axis=1, keepdims=True))
    out_ref[...] = mix * jnp.dot(hidden, down_ref[...], preferred_element_type=jnp.float32)


def side_branch(normed, vector, both, down):
    count, width = normed.shape
    return pl.pallas_call(
        side_kernel,
        out_shape=jax.ShapeDtypeStruct((count, width), jnp.float32),
        cost_estimate=cost(2 * count * width * 768, 4e6),
        name="side_branch",
    )(normed, vector.reshape(1, width), both, down)


def combine_kernel(back_ref, hi_ref, lo_ref, side_ref, *rest):
    back = back_ref[...]
    total = jnp.dot(hi_ref[...], back, preferred_element_type=jnp.float32)
    total += jnp.dot(lo_ref[...], back, preferred_element_type=jnp.float32)
    rest[-1][...] = (total + side_ref[...]).astype(jnp.bfloat16)


def combine_piece(back, hi, lo, side, held, at):
    total, wide = back.shape
    count, width = side.shape
    more = [] if held is None else [held]
    return pl.pallas_call(
        combine_kernel,
        grid=(1,),
        in_specs=[
            pl.BlockSpec((total, wide), lambda i: (0, 0)),
            pl.BlockSpec((count, total), lambda i: (0, 0)),
            pl.BlockSpec((count, total), lambda i: (0, 0)),
            pl.BlockSpec((count, wide), lambda i: (0, at)),
        ]
        + [pl.BlockSpec(memory_space=pl.ANY)] * len(more),
        out_specs=pl.BlockSpec((count, wide), lambda i: (0, at)),
        out_shape=jax.ShapeDtypeStruct((count, width), jnp.bfloat16),
        input_output_aliases={4: 0} if more else {},
        cost_estimate=cost(4 * count * total * wide, 2 * total * wide + 4 * count * total + 6 * count * wide),
        name=f"combine_{at}",
    )(back, hi, lo, side, *more)


def dense_weights(dense_gate, dense_up, dense_down):
    ep, tp = lax.axis_size(EP), lax.axis_size("tp")
    t = lax.axis_index("tp")
    deep, fs = dense_gate.shape
    wide = dense_down.shape[1]
    r, q = deep // tp, fs // tp
    both = jnp.concatenate(
        [lax.dynamic_slice_in_dim(a, t * r, r, 0) for a in (dense_gate, dense_up)], axis=1
    )
    own = lax.dynamic_slice_in_dim(dense_down, t * q, q, 0).reshape(-1, 2 * fs)
    mine = jnp.concatenate([both, own, jnp.zeros((16 - r - len(own), 2 * fs), both.dtype)], axis=0)
    near = lax.all_to_all(jnp.broadcast_to(mine[None], (ep, *mine.shape)), EP, split_axis=0, concat_axis=0, tiled=True)
    far = lax.all_gather(near.reshape(-1, 2 * fs), "tp", axis=0, tiled=True).reshape(tp, ep, 16, 2 * fs)
    whole = far[:, :, :r].transpose(1, 0, 2, 3).reshape(ep * deep, 2 * fs)
    down = far[:, :, r : r + len(own)].reshape(tp, ep, q, wide).transpose(0, 2, 1, 3).reshape(fs, ep * wide)
    return whole, down


def on_device(
    tokens, norm_gain, expert_ids, gate_weights, w_gate, w_up, w_down, dense_gate, dense_up, dense_down, mix_vector
):
    count, topk = expert_ids.shape
    width = tokens.shape[1]
    groups = lax.axis_size(EP)
    cap = 2 * count * topk // groups
    turned = [w[0].T for w in (w_gate, w_up, w_down)]
    both = lax.all_gather(jnp.concatenate(turned[:2], axis=1), "tp", axis=0, tiled=True)
    down = lax.all_gather(turned[2], "tp", axis=0, tiled=True)
    buffer, normed, dest = dispatch(tokens, norm_gain, expert_ids.T, groups, cap)
    arrived = lax.all_to_all(buffer.reshape(groups, cap, width), EP, split_axis=0, concat_axis=0, tiled=True)
    hi, lo = weigh(dest, gate_weights.T, groups * cap)
    side = side_branch(normed, mix_vector, *dense_weights(dense_gate, dense_up, dense_down))
    hidden = hidden_units(arrived.reshape(groups * cap, width), both)
    mixed = None
    for at in range(PIECES):
        piece = down_piece(hidden, down, at, PIECES)
        back = lax.all_to_all(piece.reshape(groups, cap, -1), EP, split_axis=0, concat_axis=0, tiled=True)
        mixed = combine_piece(back.reshape(groups * cap, -1), hi, lo, side, mixed, at)
    return mixed


def solution(mesh):
    torus = Mesh(mesh.devices.reshape(4, 4, mesh.shape["tp"]), ("ep_0", "ep_1", "tp"))
    return jax.shard_map(
        on_device,
        mesh=torus,
        in_specs=(
            P(EP_TP, None),
            P(),
            P(EP_TP, None),
            P(EP_TP, None),
            P(EP, None, "tp"),
            P(EP, None, "tp"),
            P(EP, None, "tp"),
            P(EP, None),
            P(EP, None),
            P(None, EP),
            P(),
        ),
        out_specs=P(EP_TP, None),
        check_vma=False,
    )
```

```python
import functools

import jax
import jax.numpy as jnp
from jax import lax
from jax.experimental import pallas as pl
from jax.experimental.pallas import tpu as pltpu
from jax.sharding import Mesh
from jax.sharding import PartitionSpec as P


EP = ("y", "x")
TP = ("z", "core")
ALL = EP + TP
EPS = 1e-06
NT = (((1,), (1,)), ((), ()))
GROUPS = (
    ((2, 1), (2, 3), (0, 2)),
    ((1, 2), (3, 2), (2, 0)),
    ((2, 2), (1, 1), (3, 3), (1, 3), (3, 1)),
    ((0, 1), (1, 0), (0, 3), (3, 0), (0, 0)),
)
SHIFTS = tuple(s for g in GROUPS for s in g)
MIB = 1 << 20


def cost(flops, moved):
    return pl.CostEstimate(flops=int(flops), bytes_accessed=int(moved), transcendentals=0)


def whole(shape):
    return pl.BlockSpec(shape, lambda *_: (0,) * len(shape))


def bf16(*shape):
    return jax.ShapeDtypeStruct(shape, jnp.bfloat16)


def one_row(a):
    return jnp.concatenate([a[i : i + 1, :] for i in range(a.shape[0])], axis=1)


def dispatch_kernel(
    groups, cap, at_ref, tok_ref, gain_ref, ids_ref, dg_ref, du_ref, dd_ref, buf_ref, normed_ref, place_ref, dest_ref, extra_ref
):
    step = pl.program_id(0)
    count = tok_ref.shape[0]
    nx = 4

    @pl.when(step == 0)
    def _():
        values = tok_ref[...].astype(jnp.float32)
        scale = lax.rsqrt(jnp.mean(values * values, axis=1, keepdims=True) + EPS)
        normed_ref[...] = (values * scale * gain_ref[...]).astype(jnp.bfloat16)
        ids = ids_ref[...]
        expert = lax.broadcasted_iota(jnp.int32, (groups, count), 0)
        hot = [jnp.where(ids[k : k + 1, :] == expert, 1.0, 0.0) for k in range(2)]
        row = lax.broadcasted_iota(jnp.int32, (count, count), 0)
        col = lax.broadcasted_iota(jnp.int32, (count, count), 1)
        earlier = jnp.where(row < col, 1.0, 0.0).astype(jnp.bfloat16)
        before = jnp.dot((hot[0] + hot[1]).astype(jnp.bfloat16), earlier, preferred_element_type=jnp.float32)
        slots = [jnp.sum(before * h, axis=0, keepdims=True).astype(jnp.int32) for h in hot]
        rest = [jnp.zeros((6, count), jnp.int32)]
        dest_ref[...] = jnp.concatenate([ids[k : k + 1, :] * cap + slots[k] for k in range(2)] + rest, axis=0)
        shift = ((ids >> 2) + nx - at_ref[0]) % nx * nx + ((ids & 3) + nx - at_ref[1]) % nx
        near = sum(jnp.where(shift == a * nx + b, k, 0) for k, (a, b) in enumerate(SHIFTS))
        place_ref[...] = jnp.concatenate([near[k : k + 1, :] * cap + slots[k] for k in range(2)] + rest, axis=0)
        fs, part = dd_ref.shape[0], dd_ref.shape[0] // 16
        unit = at_ref[2] * part + lax.broadcasted_iota(jnp.int32, (part, fs), 0)
        own = jnp.where(lax.broadcasted_iota(jnp.int32, (part, fs), 1) == unit, 1.0, 0.0).astype(jnp.bfloat16)
        shares = [lax.dot_general(own, r[...], NT, preferred_element_type=jnp.float32) for r in (dg_ref, du_ref)]
        shares += [jnp.dot(own, dd_ref[...], preferred_element_type=jnp.float32)]
        rows = [one_row(v) for v in shares]
        extra_ref[...] = jnp.concatenate(rows + [jnp.zeros((5, rows[0].shape[1]), jnp.float32)], axis=0).astype(jnp.bfloat16)

    many, _, _ = buf_ref.shape
    place = step * many * cap + lax.broadcasted_iota(jnp.int32, (many * cap, count), 0)
    chosen = (place == dest_ref[0:1, :]) | (place == dest_ref[1:2, :])
    pick = jnp.where(chosen, 1.0, 0.0).astype(jnp.bfloat16)
    rows = jnp.dot(pick, normed_ref[...], preferred_element_type=jnp.float32).astype(jnp.bfloat16)
    for i in range(many):
        buf_ref[i, :cap, :] = rows[i * cap : (i + 1) * cap, :]
        buf_ref[i, cap:, :] = extra_ref[...]


def dispatch(at, tokens, gain, ids_t, dense, groups, cap):
    count, width = tokens.shape
    steps, tall = 4, cap + 8
    return pl.pallas_call(
        functools.partial(dispatch_kernel, groups, cap),
        grid=(steps,),
        in_specs=[pl.BlockSpec(memory_space=pltpu.SMEM)]
        + [whole(a) for a in ((count, width), (1, width), (2, count))]
        + [whole(d.shape) for d in dense],
        out_specs=[
            pl.BlockSpec((groups // steps, tall, width), lambda i: (i, 0, 0)),
            whole((count, width)),
            whole((8, count)),
        ],
        out_shape=[bf16(groups, tall, width), bf16(count, width), jax.ShapeDtypeStruct((8, count), jnp.int32)],
        scratch_shapes=[pltpu.VMEM((8, count), jnp.int32), pltpu.VMEM((8, width), jnp.bfloat16)],
        cost_estimate=cost(2 * groups * cap * count * width, 8 * groups * cap * width),
        name="dispatch",
    )(at, tokens, gain.reshape(1, width), ids_t, *dense)


def weigh_kernel(dest_ref, gates_ref, hi_ref, lo_ref):
    count, total = hi_ref.shape
    dest = dest_ref[...].astype(jnp.float32).T
    gates = jnp.concatenate([gates_ref[...], jnp.zeros((6, count), jnp.float32)], axis=0).T
    place = lax.broadcasted_iota(jnp.int32, (count, total), 1).astype(jnp.float32)
    weight = sum(jnp.where(place == dest[:, k : k + 1], gates[:, k : k + 1], 0.0) for k in range(2))
    hi = weight.astype(jnp.bfloat16)
    hi_ref[...] = hi
    lo_ref[...] = (weight - hi.astype(jnp.float32)).astype(jnp.bfloat16)


def weigh(dest, gates_t, total):
    count = gates_t.shape[1]
    return pl.pallas_call(
        weigh_kernel,
        out_shape=[bf16(count, total)] * 2,
        cost_estimate=cost(2e9, 4 * count * total),
        name="weigh",
    )(dest, gates_t)


def hidden_kernel(rows_ref, gate_ref, up_ref, out_ref):
    groups, cap, width = rows_ref.shape
    part = 4
    for at in range(0, groups, part):
        rows = rows_ref[at : at + part].reshape(part * cap, width)
        gate = lax.dot_general(rows, gate_ref[...], NT, preferred_element_type=jnp.float32)
        upper = lax.dot_general(rows, up_ref[...], NT, preferred_element_type=jnp.float32)
        out_ref[at * cap : (at + part) * cap, :] = (jax.nn.silu(gate) * upper).astype(jnp.bfloat16)


def hidden_units(arrived, weights, cap):
    groups, _, width = arrived.shape
    units, block = weights.shape[0], 256
    total = groups * cap
    return pl.pallas_call(
        hidden_kernel,
        grid=(units // block,),
        in_specs=[
            pl.BlockSpec((groups, cap, width), lambda i: (0, 0, 0)),
            pl.BlockSpec((block, width), lambda i: (i, 0)),
            pl.BlockSpec((block, width), lambda i: (i, 1)),
        ],
        out_specs=pl.BlockSpec((total, block), lambda i: (0, i)),
        out_shape=bf16(total, units),
        cost_estimate=cost(4 * total * width * units, 2 * total * width + 4 * units * width + 2 * total * units),
        name="hidden_units",
    )(arrived, weights, weights)


def down_kernel(many, at_ref, *refs):
    rows, down_ref, outs = refs[:many], refs[many], refs[many + 1 :]
    cap = outs[0].shape[0]
    hidden = jnp.concatenate([r[...] for r in rows], axis=0)
    result = jnp.dot(hidden, down_ref[...], preferred_element_type=jnp.float32).astype(jnp.bfloat16)
    for i, out in enumerate(outs):
        out[...] = result[i * cap : (i + 1) * cap, :]


def down_group(source, hidden, weights, cap, start, many):
    units, width = weights.shape[0], weights.shape[1] // 3
    wide = 512
    skip = 2 * width // wide
    return pl.pallas_call(
        functools.partial(down_kernel, many),
        grid_spec=pltpu.PrefetchScalarGridSpec(
            num_scalar_prefetch=1,
            grid=(width // wide,),
            in_specs=[pl.BlockSpec((cap, units), lambda i, at, k=k: (at[start + k], 0)) for k in range(many)]
            + [pl.BlockSpec((units, wide), lambda i, at: (0, skip + i))],
            out_specs=[pl.BlockSpec((cap, wide), lambda i, at: (0, i))] * many,
        ),
        out_shape=[bf16(cap, width)] * many,
        compiler_params=pltpu.CompilerParams(vmem_limit_bytes=54 * MIB),
        cost_estimate=cost(2 * many * cap * width * units, 2 * units * width + 4 * many * cap * width),
    )(source, *[hidden] * many, weights)


def side_kernel(normed_ref, vector_ref, dense_ref, out_ref):
    normed = normed_ref[...]
    gate, up, down = (jnp.concatenate([dense_ref[t, k] for t in range(dense_ref.shape[0])], axis=0) for k in range(3))
    dense_g = lax.dot_general(normed, gate, NT, preferred_element_type=jnp.float32)
    dense_u = lax.dot_general(normed, up, NT, preferred_element_type=jnp.float32)
    hidden = (jax.nn.silu(dense_g) * dense_u).astype(jnp.bfloat16)
    mix = jax.nn.sigmoid(jnp.sum(normed.astype(jnp.float32) * vector_ref[...], axis=1, keepdims=True))
    out_ref[...] = mix * jnp.dot(hidden, down, preferred_element_type=jnp.float32)


def side_branch(normed, vector, dense):
    count, width = normed.shape
    return pl.pallas_call(
        side_kernel,
        out_shape=jax.ShapeDtypeStruct((count, width), jnp.float32),
        compiler_params=pltpu.CompilerParams(vmem_limit_bytes=24 * MIB),
        cost_estimate=cost(2 * count * width * 768, 4e6),
        name="side_branch",
    )(normed, vector.reshape(1, width), dense)


def combine_kernel(start, many, *refs):
    backs, (hi_ref, lo_ref, add_ref, out_ref) = refs[:many], refs[many:]
    cap = backs[0].shape[0]
    back = jnp.concatenate([b[...] for b in backs], axis=0)
    at = slice(start * cap, (start + many) * cap)
    total = add_ref[...] + jnp.dot(hi_ref[:, at], back, preferred_element_type=jnp.float32)
    total += jnp.dot(lo_ref[:, at], back, preferred_element_type=jnp.float32)
    out_ref[...] = total.astype(out_ref.dtype)


def combine(backs, hi, lo, add, start, dtype):
    many, (cap, width) = len(backs), backs[0].shape
    count, total = hi.shape
    wide = 1024
    column = lambda i: (0, i)
    return pl.pallas_call(
        functools.partial(combine_kernel, start, many),
        grid=(width // wide,),
        in_specs=[pl.BlockSpec((cap, wide), column)] * many
        + [whole((count, total))] * 2
        + [pl.BlockSpec((count, wide), column)],
        out_specs=pl.BlockSpec((count, wide), column),
        out_shape=jax.ShapeDtypeStruct((count, width), dtype),
        compiler_params=pltpu.CompilerParams(vmem_limit_bytes=20 * MIB),
        cost_estimate=cost(4 * count * many * cap * width, 2 * many * cap * width + 8 * count * width),
    )(*backs, hi, lo, add)


def shifted(a, shift):
    if shift == (0, 0):
        return a
    dy, dx = shift
    ny, nx = lax.axis_size("y"), lax.axis_size("x")
    pairs = [(y * nx + x, (y + dy) % ny * nx + (x + dx) % nx) for y in range(ny) for x in range(nx)]
    return lax.ppermute(a, EP, pairs)


def on_device(
    tokens, norm_gain, expert_ids, gate_weights, w_gate, w_up, w_down, dense_gate, dense_up, dense_down, mix_vector
):
    count, topk = expert_ids.shape
    width = tokens.shape[1]
    groups, tp = lax.axis_size(EP), lax.axis_size(TP)
    ny, nx = lax.axis_size("y"), lax.axis_size("x")
    y, x = lax.axis_index("y"), lax.axis_index("x")
    cap = 2 * count * topk // groups
    weights = jnp.concatenate([w[0].T for w in (w_gate, w_up, w_down)], axis=1)
    weights = lax.all_gather(weights, TP, axis=0, tiled=True)

    at = jnp.stack([y, x, lax.axis_index(TP)]).astype(jnp.int32)
    dense = (dense_gate, dense_up, dense_down)
    buffer, normed, dest = dispatch(at, tokens, norm_gain, expert_ids.T, dense, groups, cap)
    arrived = lax.all_to_all(buffer, EP, split_axis=0, concat_axis=0, tiled=True)
    hi, lo = weigh(dest, gate_weights.T, groups * cap)
    part = dense_down.shape[0] // tp
    dense = arrived[:, cap : cap + 3].reshape(groups, 3, part, -1).transpose(1, 2, 0, 3)
    dense = lax.all_gather(dense.reshape(3 * part, width), TP, axis=0, tiled=True)
    dense = dense.reshape(tp, 3, part, width)
    hidden = hidden_units(arrived, weights, cap)
    down_y, down_x = (jnp.array(v, jnp.int32) for v in zip(*SHIFTS))
    source = ((y - down_y) % ny * nx + (x - down_x) % nx).astype(jnp.int32)
    backs = []
    for group in GROUPS:
        results = down_group(source, hidden, weights, cap, len(backs), len(group))
        backs += [shifted(a, (-s[0] % ny, -s[1] % nx)) for a, s in zip(results, group)]
    side = side_branch(normed, mix_vector, dense)
    cut = groups - len(GROUPS[-1])
    part = combine(backs[:cut], hi, lo, side, 0, jnp.float32)
    return combine(backs[cut:], hi, lo, part, cut, jnp.bfloat16)


def solution(mesh):
    tp = mesh.shape["tp"]
    torus = Mesh(mesh.devices.reshape(4, 4, tp // 2, 2), ALL)
    return jax.shard_map(
        on_device,
        mesh=torus,
        in_specs=(
            P(ALL, None),
            P(),
            P(ALL, None),
            P(ALL, None),
            P(EP, None, TP),
            P(EP, None, TP),
            P(EP, None, TP),
            P(EP, None),
            P(EP, None),
            P(None, EP),
            P(),
        ),
        out_specs=P(ALL, None),
        check_vma=False,
    )
```
